32 devices in a mesh: sp: 16 (over z, y, x), tp: 2 (over core).
Axes of the slice: x: 2, y: 2, z: 4, core: 2. Of those that a mesh axis runs over, the one named last changes fastest.
Arguments:
- value_in: bfloat16 [5760, 2048], P('sp', 'tp'), may hold values from -240 to 240
- gate_in: bfloat16 [5760, 2048], P('sp', 'tp'), may hold values from -8 to 8
- taps: float32 [31, 2048], P(None, 'tp'), may hold values from -1 to 1
- norm_gain: float32 [2048], P('tp'), may hold values from 0.1 to 1.9
- norm_bias: float32 [2048], P('tp'), may hold values from -3 to 3
- proj_weight: bfloat16 [2048, 4096], P('tp', 'sp'), may hold values from -0.125 to 0.125
- out_grad: bfloat16 [5760, 4096], P('sp'), may hold values from -6 to 6
Outputs:
- value_grad: bfloat16 [5760, 2048], P('sp', 'tp')
- gate_grad: bfloat16 [5760, 2048], P('sp', 'tp')
- tap_grad: float32 [31, 2048], P(None, 'tp')
- gain_grad: float32 [2048], P('tp')
- bias_grad: float32 [2048], P('tp')
- weight_grad: float32 [2048, 4096], P('tp', 'sp')
The draws below stay inside these ranges and needn't reach their ends.
All inputs are finite; a program needn't handle non-finite values.
Results may differ from the reference program's by a relative error of at most 0.0051.
Values may be sent and summed in bfloat16 or wider, within the bound.
A program may use at most 64 MiB of HBM per device.

```python
import math
import jax
import jax.numpy as jnp
from jax import lax

MODEL = 4096
CHANNELS = 2048
TAPS = 31
TOKENS = 5760


def draw_value_in(key, part):
    first, second = jax.random.split(key, 2)
    chan = jnp.exp(jnp.linspace(0.0, math.log(10.0), CHANNELS)) * jax.random.uniform(second, (CHANNELS,), jnp.float32, 0.5, 2.0)
    along = jnp.exp(jnp.linspace(0.0, math.log(3.0), TOKENS))[:, None]
    base = jnp.clip(jax.random.normal(first, (TOKENS, CHANNELS), jnp.float32), -4.0, 4.0)
    return jnp.clip(base * chan[None, :] * along, -240.0, 240.0).astype(jnp.bfloat16)


def with_spikes(drawn, rng, source, target, blocks, factor):
    def block_of(position):
        return (jnp.arange(drawn.shape[position]) // (drawn.shape[position] // blocks)).reshape((-1,) + (1,) * (drawn.ndim - 1 - position))

    one_side = jax.random.permutation(rng, blocks)[block_of(target)]
    second = (block_of(target) + blocks // 2) % blocks
    return jnp.where((block_of(source) == one_side) | (block_of(source) == second), factor * drawn, drawn)


def levels(rng, shape, cuts, smallest, largest):
    loudness = 1.0
    for axis_at, shards_of in cuts:
        heights = jax.random.uniform(jax.random.fold_in(jax.random.fold_in(rng, 6), axis_at), (shards_of,), jnp.float32, smallest / len(cuts), largest / len(cuts))
        loudness = loudness * jnp.repeat(jnp.exp(heights), shape[axis_at] // shards_of).reshape((-1,) + (1,) * (len(shape) - 1 - axis_at))
    return loudness


def gaussian(key, dims, width, most, cuts=(), dtype=jnp.bfloat16):
    loudness = levels(key, dims, cuts, -0.22, 0.18) if cuts else 1.0
    values = jax.random.normal(key, dims, jnp.float32) * width * loudness
    return jnp.minimum(jnp.maximum(values, -most), most).astype(dtype)


def heavy_noise(stream_key, shape, scale, reach, cuts, heavy, kind=jnp.bfloat16):
    values = scale * jax.random.normal(stream_key, shape, jnp.float32)
    if cuts:
        values = values * levels(stream_key, shape, cuts, -0.22, 0.18)
    return jnp.clip(with_spikes(values, jax.random.fold_in(stream_key, 3), *heavy), -reach, reach).astype(kind)


def setup_inputs(seed: int = 0) -> dict:
    streams_of = jax.random.split(jax.random.key(seed), 8)
    return {
        "value_in": draw_value_in(jax.random.fold_in(streams_of[7], 71), 0),
        "gate_in": gaussian(streams_of[1], (TOKENS, CHANNELS), 2.0, 8.0, ((0, 16), (1, 2))),
        "taps": gaussian(streams_of[2], (TAPS, CHANNELS), TAPS ** -0.5, 1.0, ((1, 2),), jnp.float32),
        "norm_gain": jnp.clip(1.0 + 0.18 * jax.random.normal(streams_of[3], (CHANNELS,), jnp.float32), 0.1, 1.9),
        "norm_bias": gaussian(streams_of[4], (CHANNELS,), 0.5, 3.0, ((0, 2),), jnp.float32),
        "proj_weight": gaussian(streams_of[5], (CHANNELS, MODEL), CHANNELS ** -0.5, 0.125, ((0, 2), (1, 16))),
        "out_grad": heavy_noise(streams_of[6], (TOKENS, MODEL), 1.0, 6.0, ((0, 16),), (0, 1, 16, 2.0)),
    }


def reference(value_in, gate_in, taps, norm_gain, norm_bias, proj_weight, out_grad):
    f32 = jnp.float32
    rows = value_in.shape[0]
    span = taps.shape[0]
    half = span // 2
    width_all = value_in.shape[1]
    gate_sig = jax.nn.sigmoid(gate_in.astype(f32))
    value_f = value_in.astype(f32)
    mixed = (value_f * gate_sig).astype(jnp.bfloat16)
    padded = jnp.pad(mixed.astype(f32), ((half, half), (0, 0)))
    conv = jnp.zeros((rows, width_all), f32)
    for k in range(span):
        conv = conv + taps[k] * padded[k:k + rows]
    mean = lax.optimization_barrier(jnp.sum(conv, axis=1)) / width_all
    centred = conv - mean[:, None]
    spread = lax.optimization_barrier(jnp.sum(centred * centred, axis=1)) / width_all
    inv = lax.rsqrt(spread + 1e-06)
    normed = centred * inv[:, None]
    pre = normed * norm_gain + norm_bias
    act = jax.nn.silu(pre).astype(jnp.bfloat16)
    act_grad = lax.dot_general(out_grad, proj_weight, (((1,), (1,)), ((), ())), preferred_element_type=f32)
    weight_grad = lax.dot_general(act, out_grad, (((0,), (0,)), ((), ())), preferred_element_type=f32)
    sig_pre = jax.nn.sigmoid(pre)
    pre_grad = act_grad * sig_pre * (1.0 + pre * (1.0 - sig_pre))
    gain_grad = lax.optimization_barrier(jnp.sum(pre_grad * normed, axis=0))
    bias_grad = lax.optimization_barrier(jnp.sum(pre_grad, axis=0))
    normed_grad = pre_grad * norm_gain
    first = lax.optimization_barrier(jnp.sum(normed_grad, axis=1)) / width_all
    second = lax.optimization_barrier(jnp.sum(normed_grad * normed, axis=1)) / width_all
    conv_grad = inv[:, None] * (normed_grad - first[:, None] - normed * second[:, None])
    tap_grad = jnp.stack([lax.optimization_barrier(jnp.sum(conv_grad * padded[k:k + rows], axis=0)) for k in range(span)])
    grad_pad = jnp.pad(conv_grad, ((half, half), (0, 0)))
    mixed_grad = jnp.zeros((rows, width_all), f32)
    for k in range(span):
        mixed_grad = mixed_grad + taps[k] * grad_pad[2 * half - k:2 * half - k + rows]
    value_grad = (mixed_grad * gate_sig).astype(jnp.bfloat16)
    gate_grad = (mixed_grad * value_f * gate_sig * (1.0 - gate_sig)).astype(jnp.bfloat16)
    return (value_grad, gate_grad, tap_grad, gain_grad, bias_grad, weight_grad)
```

```python
import jax
import jax.numpy as jnp
from jax import lax
from jax.sharding import PartitionSpec as P


def padded_rows(cells, width):
    count = lax.axis_size("sp")
    ends = count - 1
    rows = cells.shape[0]
    before = lax.ppermute(cells[rows - width :], "sp", [(i, i + 1) for i in range(ends)])
    after = lax.ppermute(cells[:width], "sp", [(i + 1, i) for i in range(ends)])
    return jnp.concatenate([before, cells, after], axis=0)


def on_device(value_in, gate_in, taps, norm_gain, norm_bias, proj_weight, out_grad):
    f32, bf16 = jnp.float32, jnp.bfloat16
    rows, local_width = value_in.shape
    span = taps.shape[0]
    half = span // 2
    tp = lax.axis_size("tp")
    count = lax.axis_size("sp")
    inner = 1 << ((count.bit_length() - 1) // 2)
    outer = count // inner
    width_all = local_width * tp
    block = proj_weight.shape[1]
    me = lax.axis_index("sp")
    plane, place = me // inner, me % inner
    core = lax.axis_index("tp")

    def swap(array, d):
        return lax.ppermute(
            array, "sp", [(i, i - i % inner + ((i % inner) ^ d)) for i in range(count)]
        )

    def shift(array, e):
        return lax.ppermute(array, "sp", [(i, (i + e * inner) % count) for i in range(count)])

    def across(array, t):
        return lax.ppermute(array, "tp", [(c, c ^ t) for c in range(tp)])

    def tp_sum(array):
        return array + sum(across(array, t) for t in range(1, tp))

    gate_sig = jax.nn.sigmoid(gate_in.astype(f32))
    value_f = value_in.astype(f32)
    mixed = (value_f * gate_sig).astype(bf16)
    padded = padded_rows(mixed, half).astype(f32)

    blocks = out_grad.reshape(rows, outer, inner * block)
    blocks = jnp.concatenate([blocks, blocks], axis=1)
    blocks = lax.dynamic_slice_in_dim(blocks, plane, outer, axis=1).reshape(
        rows, outer, inner, block
    )

    def columns_of(where):
        picked = lax.dynamic_index_in_dim(blocks, where, axis=2, keepdims=False)
        return picked.reshape(rows, outer * block)

    piece = outer * block // tp
    own_columns = columns_of(place)
    arrived = []
    for d in range(1, inner):
        mine = lax.dynamic_slice_in_dim(columns_of(place ^ d), core * piece, piece, axis=1)
        arrived.append(swap(mine, d))
    weights = [proj_weight] + [shift(proj_weight, -e) for e in range(1, outer)]
    weight_cols = jnp.concatenate(weights, axis=1)
    cotangents = [own_columns]
    for got in arrived:
        parts = jnp.stack([got] + [across(got, t) for t in range(1, tp)])
        cotangents.append(
            jnp.concatenate(
                [
                    lax.dynamic_index_in_dim(parts, core ^ j, axis=0, keepdims=False)
                    for j in range(tp)
                ],
                axis=1,
            )
        )

    partial = [
        lax.dot_general(c, weight_cols, (((1,), (1,)), ((), ())), preferred_element_type=f32)
        for c in cotangents
    ]
    act_grad = partial[0]
    for d in range(1, inner):
        act_grad = act_grad + swap(partial[d].astype(bf16), d).astype(f32)

    conv = jnp.zeros((rows, local_width), f32)
    for k in range(span):
        conv = conv + taps[k] * padded[k : k + rows]
    mean = tp_sum(jnp.sum(conv, axis=1)) / width_all
    centred = conv - mean[:, None]
    spread = tp_sum(jnp.sum(centred * centred, axis=1)) / width_all
    inv = lax.rsqrt(spread + 1e-06)
    normed = centred * inv[:, None]
    pre = normed * norm_gain + norm_bias
    sig_pre = jax.nn.sigmoid(pre)
    act = (pre * sig_pre).astype(bf16)
    acts = [act] + [swap(act, d) for d in range(1, inner)]

    pre_grad = act_grad * sig_pre * (1.0 + pre * (1.0 - sig_pre))
    normed_grad = pre_grad * norm_gain
    sums = tp_sum(
        jnp.stack([jnp.sum(normed_grad, axis=1), jnp.sum(normed_grad * normed, axis=1)])
    )
    first, second = sums[0], sums[1]
    conv_grad = inv[:, None] * (
        normed_grad - first[:, None] / width_all - normed * second[:, None] / width_all
    )
    extended = padded_rows(conv_grad, half)
    tap_local = jnp.stack([jnp.sum(conv_grad * padded[k : k + rows], axis=0) for k in range(span)])
    gain_local = jnp.sum(pre_grad * normed, axis=0)
    bias_local = jnp.sum(pre_grad, axis=0)
    small = jnp.concatenate([tap_local, gain_local[None], bias_local[None]], axis=0)
    small = small + sum(swap(small, d) for d in range(1, inner))
    small = small + sum(shift(small, e) for e in range(1, outer))
    tap_grad, gain_grad, bias_grad = small[:span], small[span], small[span + 1]

    mixed_grad = jnp.zeros((rows, local_width), f32)
    for k in range(span):
        mixed_grad = mixed_grad + taps[k] * extended[2 * half - k : 2 * half - k + rows]
    value_grad = (mixed_grad * gate_sig).astype(bf16)
    gate_grad = (mixed_grad * value_f * gate_sig * (1.0 - gate_sig)).astype(bf16)

    weight_part = lax.dot_general(
        jnp.concatenate(acts, axis=0),
        jnp.concatenate(cotangents, axis=0),
        (((0,), (0,)), ((), ())),
        preferred_element_type=f32,
    )
    weight_grad = weight_part[:, :block]
    for e in range(1, outer):
        sent = weight_part[:, e * block : (e + 1) * block].astype(bf16)
        weight_grad = weight_grad + shift(sent, e).astype(f32)
    return (value_grad, gate_grad, tap_grad, gain_grad, bias_grad, weight_grad)


def solution(mesh):
    return jax.shard_map(
        on_device,
        mesh=mesh,
        in_specs=(
            P("sp", "tp"),
            P("sp", "tp"),
            P(None, "tp"),
            P("tp"),
            P("tp"),
            P("tp", "sp"),
            P("sp", None),
        ),
        out_specs=(P("sp", "tp"), P("sp", "tp"), P(None, "tp"), P("tp"), P("tp"), P("tp", "sp")),
        check_vma=False,
    )
```

```python
import jax
import jax.numpy as jnp
from jax import lax
from jax.sharding import PartitionSpec as P


def padded_rows(cells, width):
    count = lax.axis_size("sp")
    ends = count - 1
    rows = cells.shape[0]
    before = lax.ppermute(cells[rows - width :], "sp", [(i, i + 1) for i in range(ends)])
    after = lax.ppermute(cells[:width], "sp", [(i + 1, i) for i in range(ends)])
    return jnp.concatenate([before, cells, after], axis=0)


def compute(value_in, gate_in, taps, norm_gain, norm_bias, proj_weight, out_grad):
    f32, bf16 = jnp.float32, jnp.bfloat16
    rows, local_width = value_in.shape
    span = taps.shape[0]
    half = span // 2
    tp = lax.axis_size("tp")
    count = lax.axis_size("sp")
    inner = 1 << ((count.bit_length() - 1) // 2)
    outer = count // inner
    width_all = local_width * tp
    block = proj_weight.shape[1]
    me = lax.axis_index("sp")
    plane, place = me // inner, me % inner
    core = lax.axis_index("tp")

    def swap(array, d):
        return lax.ppermute(
            array, "sp", [(i, i - i % inner + ((i % inner) ^ d)) for i in range(count)]
        )

    def shift(array, e):
        return lax.ppermute(array, "sp", [(i, (i + e * inner) % count) for i in range(count)])

    def across(array, t):
        return lax.ppermute(array, "tp", [(c, c ^ t) for c in range(tp)])

    def tp_sum(array):
        return array + sum(across(array, t) for t in range(1, tp))

    gate_sig = jax.nn.sigmoid(gate_in.astype(f32))
    value_f = value_in.astype(f32)
    mixed = (value_f * gate_sig).astype(bf16)
    padded = padded_rows(mixed, half).astype(f32)

    def columns_of(where, first, blocks):
        return jnp.concatenate(
            [
                lax.dynamic_slice_in_dim(
                    out_grad,
                    (((plane + first + e) % outer) * inner + where) * block,
                    block,
                    axis=1,
                )
                for e in range(blocks)
            ],
            axis=1,
        )

    share = outer // tp
    own_columns = columns_of(place, 0, outer)
    arrived = [swap(columns_of(place ^ d, core * share, share), d) for d in range(1, inner)]
    weights = [proj_weight] + [shift(proj_weight, -e) for e in range(1, outer)]
    weight_cols = jnp.concatenate(weights, axis=1)
    cotangents = [own_columns]
    for got in arrived:
        parts = jnp.stack([got] + [across(got, t) for t in range(1, tp)])
        cotangents.append(
            jnp.concatenate(
                [
                    lax.dynamic_index_in_dim(parts, core ^ j, axis=0, keepdims=False)
                    for j in range(tp)
                ],
                axis=1,
            )
        )

    conv = jnp.zeros((rows, local_width), f32)
    for k in range(span):
        conv = conv + taps[k] * padded[k : k + rows]
    mean = tp_sum(jnp.sum(conv, axis=1)) / width_all
    centred = conv - mean[:, None]
    spread = tp_sum(jnp.sum(centred * centred, axis=1)) / width_all
    inv = lax.rsqrt(spread + 1e-06)
    normed = centred * inv[:, None]
    pre = normed * norm_gain + norm_bias
    sig_pre = jax.nn.sigmoid(pre)
    act = (pre * sig_pre).astype(bf16)
    acts = [act] + [swap(act, d) for d in range(1, inner)]

    partial = [
        lax.dot_general(c, weight_cols, (((1,), (1,)), ((), ())), preferred_element_type=f32)
        for c in cotangents
    ]
    act_grad = partial[0]
    sending = lax.optimization_barrier(([p.astype(bf16) for p in partial[1:]], acts))[0]
    for d in range(1, inner):
        got = swap(sending[d - 1], d)
        act_grad = act_grad + got.astype(f32)

    pre_grad = act_grad * sig_pre * (1.0 + pre * (1.0 - sig_pre))
    normed_grad = pre_grad * norm_gain
    sums = tp_sum(
        jnp.stack([jnp.sum(normed_grad, axis=1), jnp.sum(normed_grad * normed, axis=1)])
    )
    first, second = sums[0], sums[1]
    conv_grad = inv[:, None] * (
        normed_grad - first[:, None] / width_all - normed * second[:, None] / width_all
    )
    extended = lax.optimization_barrier(padded_rows(conv_grad, half))
    tap_local = jnp.stack([jnp.sum(conv_grad * padded[k : k + rows], axis=0) for k in range(span)])
    gain_local = jnp.sum(pre_grad * normed, axis=0)
    bias_local = jnp.sum(pre_grad, axis=0)
    small = jnp.concatenate([tap_local, gain_local[None], bias_local[None]], axis=0)
    small = small + sum(swap(small, d) for d in range(1, inner))
    small = small + sum(shift(small, e) for e in range(1, outer))
    tap_grad, gain_grad, bias_grad = small[:span], small[span], small[span + 1]

    mixed_grad = jnp.zeros((rows, local_width), f32)
    for k in range(span):
        mixed_grad = mixed_grad + taps[k] * extended[2 * half - k : 2 * half - k + rows]
    value_grad = (mixed_grad * gate_sig).astype(bf16)
    gate_grad = (mixed_grad * value_f * gate_sig * (1.0 - gate_sig)).astype(bf16)

    weight_part = lax.dot_general(
        jnp.concatenate(acts, axis=0),
        jnp.concatenate(cotangents, axis=0),
        (((0,), (0,)), ((), ())),
        preferred_element_type=f32,
    )
    weight_grad = weight_part[:, :block]
    for e in range(1, outer):
        sent = weight_part[:, e * block : (e + 1) * block].astype(bf16)
        got = shift(sent, e)
        weight_grad = weight_grad + got.astype(f32)
    return (value_grad, gate_grad, tap_grad, gain_grad, bias_grad, weight_grad)


def solution(mesh):
    return jax.shard_map(
        compute,
        mesh=mesh,
        in_specs=(
            P("sp", "tp"),
            P("sp", "tp"),
            P(None, "tp"),
            P("tp"),
            P("tp"),
            P("tp", "sp"),
            P("sp", None),
        ),
        out_specs=(P("sp", "tp"), P("sp", "tp"), P(None, "tp"), P("tp"), P("tp"), P("tp", "sp")),
        check_vma=False,
    )
```
